32 devices in a mesh: ep: 16 (over z, y, x), tp: 2 (over core).
Axes of the slice: x: 2, y: 2, z: 4, core: 2. Of those that a mesh axis runs over, the one named last changes fastest.
Arguments:
- residual: bfloat16 [256, 2048], P(('ep', 'tp')), may hold values from -6 to 6
- query_latent: bfloat16 [256, 8, 512], P(('ep', 'tp')), may hold values from -40 to 40
- query_rotary: bfloat16 [256, 8, 32], P(('ep', 'tp')), may hold values from -6 to 6
- latent_new: bfloat16 [256, 512], P(('ep', 'tp')), may hold values from -16 to 16
- rotary_new: bfloat16 [256, 32], P(('ep', 'tp')), may hold values from -6 to 6
- latent_cache: bfloat16 [256, 256, 512], P(('ep', 'tp')), may hold values from -16 to 16
- rotary_cache: bfloat16 [256, 256, 32], P(('ep', 'tp')), may hold values from -6 to 6
- lengths: int32 [256], P(('ep', 'tp')), may hold values from 32 to 256, as said below
- value_up: bfloat16 [512, 8, 64], replicated, may hold values from -1 to 1
- out_proj: bfloat16 [512, 2048], replicated, may hold values from -0.5 to 0.5
- attn_gain: bfloat16 [2048], replicated, may hold values from 0.099609375 to 1.8984375
- mix_gate: bfloat16 [2048], replicated, may hold values from -0.125 to 0.125
- dense_w_gate: bfloat16 [2048, 2048], P(None, 'ep'), may hold values from -0.125 to 0.125
- dense_w_up: bfloat16 [2048, 2048], P(None, 'ep'), may hold values from -0.125 to 0.125
- dense_w_down: bfloat16 [2048, 2048], P('ep'), may hold values from -0.5 to 0.5
- expert_ids: int32 [256, 6], P(('ep', 'tp')), may hold values from 0 to 15, all different within a row; in each aligned block of 16 rows (0 to 15, 16 to 31, ...) at most 12 rows name the same one
- expert_scores: float32 [256, 6], P(('ep', 'tp')), may hold values from 0.1 to 5
- expert_gate: bfloat16 [16, 2048, 512], P('ep', None, 'tp'), may hold values from -0.125 to 0.125
- expert_up: bfloat16 [16, 2048, 512], P('ep', None, 'tp'), may hold values from -0.125 to 0.125
- expert_down: bfloat16 [16, 512, 2048], P('ep', 'tp'), may hold values from -1 to 1
- out_gain: bfloat16 [2048], replicated, may hold values from 0.099609375 to 1.8984375
Outputs:
- layer_out: bfloat16 [256, 2048], P(('ep', 'tp'))
The draws below stay inside these ranges and needn't reach their ends.
Inputs may be any that keep to these rules, and one draw needn't show every extreme that they name: `expert_ids`: within each aligned block of 16 rows (the sequences of one ep index) no expert is named by more than 12 rows, a bound that some block reaches; a row names 6 different experts. `lengths`: some sequence has exactly 256 cached positions.
All inputs are finite; a program needn't handle non-finite values.
Results may differ from the reference program's by a relative error of at most 0.018.
Values may be sent and summed in bfloat16 or wider, within the bound.
No kernel may reach another device: no remote copies, remote signals or barrier semaphores. Data moves between devices by JAX's collectives and lax.ppermute only.
A program may use at most 128 MiB of HBM per device.

```python
import math
import jax
import jax.numpy as jnp
import numpy as np
from jax import lax

D = 2048
H = 8
KL = 512
ROPE = 32
NOPE = 64
V = 64
FE = 512
FD = 2048
TOPK = 6
SEQ_DEV = 8
CACHE = 256
EXPERTS = 16
TOK_GROUP = 16
SEQS = 256
CAP = 12
N_TP = 2


def draw_latent_cache(key, part):
    values = jnp.clip(jax.random.normal(jax.random.fold_in(key, 1), (SEQS, CACHE, KL), jnp.float32), -6.0, 6.0)
    return values.astype(jnp.bfloat16)


def draw_query_latent(key, part):
    values = 0.5 * jnp.clip(jax.random.normal(jax.random.fold_in(key, 2), (SEQS, H, KL), jnp.float32), -6.0, 6.0)
    return values.astype(jnp.bfloat16)


def draw_lengths(key, part):
    keys = jax.random.split(jax.random.fold_in(key, 3), 3)
    short = jax.random.randint(keys[0], (SEQS,), CACHE // 8, CACHE + 1)
    full = jax.random.randint(keys[1], (SEQS,), 0, 4) == 0
    values = jnp.where(full, CACHE, short)
    values = values.at[jax.random.randint(keys[2], (), 0, SEQS)].set(CACHE)
    return values.astype(jnp.int32)


def steps_of(own_key, dims, shards, low, top_value):
    level, own = 1.0, jax.random.fold_in(own_key, 6)
    for dim, shards_of in shards:
        steps = jnp.exp(jax.random.uniform(jax.random.fold_in(own, dim), (shards_of,), jnp.float32, low / len(shards), top_value / len(shards)))
        level = level * jnp.repeat(steps, dims[dim] // shards_of).reshape([-1 if axis == dim else 1 for axis in range(len(dims))])
    return level


def routed_block(stream_key, own, number, rows, count, top, bound, slope):
    ranking = jax.random.permutation(stream_key, count)
    crowded, common = portions_of(count, rows * top, bound, slope, True), portions_of(count, rows * top, bound, slope, False)
    places = jnp.arange(count)

    def named(tallies, rotation):
        used = int((tallies > 0).sum())
        fixed = max(1, used // 4)
        shifted = fixed + (places - fixed + rotation * (used - fixed)) % max(1, count - fixed)
        return jnp.zeros((count,), jnp.int32).at[ranking[jnp.where(places < fixed, places, shifted)]].set(jnp.asarray(tallies, jnp.int32))

    tallies = jnp.where(number % 4 == 0, named(crowded, number // 4), named(common, number - number // 4 - 1))
    mixed = jax.random.permutation(jax.random.fold_in(own, 3), count)
    giver, sink = mixed[0:count // 2 * 2:2], mixed[1:count // 2 * 2:2]
    room = jnp.minimum(tallies[giver] - 1, bound - tallies[sink]) // 2
    room = jnp.where((giver == ranking[0]) | (sink == ranking[0]) | (tallies[sink] == 0), 0, jnp.maximum(room, 0))
    shifted = jax.random.randint(jax.random.fold_in(own, 4), (count // 2,), 0, 1 << 20) % (room + 1)
    tallies = tallies.at[giver].add(-shifted).at[sink].add(shifted)
    labels = jnp.searchsorted(jnp.cumsum(tallies), jnp.arange(rows * top), side="right").astype(jnp.int32)
    table = labels.reshape(top, rows).T
    table = table[jax.random.permutation(jax.random.fold_in(own, 1), rows)]
    rotation = jax.random.randint(jax.random.fold_in(own, 2), (rows, 1), 0, top)
    return jnp.take_along_axis(table, (jnp.arange(top)[None, :] + rotation) % top, axis=1)


def portions_of(amount, total, limit, lean, full):
    portions = [(1 << 20) // math.isqrt(rank ** lean) + 1 for rank in range(1, amount + 1)]
    largest = limit if full else min(limit, max(-(-total // amount), total * portions[0] // sum(portions)))
    least = 1 if total - largest >= amount - 1 else 0
    holding, spare = [largest] + [least] * (amount - 1), total - largest - least * (amount - 1)
    while spare > 0:
        free = [i for i in range(1, amount) if holding[i] < largest] or [i for i in range(1, amount) if holding[i] < limit]
        pool, left = sum([portions[i] for i in free]), spare
        for i in free:
            extra = min(limit - holding[i], max(1, left * portions[i] // pool), spare)
            holding[i] = holding[i] + extra
            spare = spare - extra
    return np.array(holding)


def normal_values(own_key, dims, deviation, bound, cuts=(), kind=jnp.bfloat16):
    level = steps_of(own_key, dims, cuts, -0.22, 0.18) if cuts else 1.0
    values = jax.random.normal(own_key, dims, jnp.float32) * deviation * level
    return jnp.minimum(jnp.maximum(values, -bound), bound).astype(kind)


def setup_inputs(seed: int = 0) -> dict:
    splits = jax.random.split(jax.random.key(seed), 22)
    residual = normal_values(splits[0], (SEQS, D), 1.0, 6.0, ((0, 32),))
    query_latent = draw_query_latent(jax.random.fold_in(splits[21], 71), 0)
    query_rotary = normal_values(splits[2], (SEQS, H, ROPE), 1.0, 6.0, ((0, 32),))
    latent_new = normal_values(splits[3], (SEQS, KL), 3.0, 16.0, ((0, 32),))
    rotary_new = normal_values(splits[4], (SEQS, ROPE), 1.0, 6.0, ((0, 32),))
    latent_cache = draw_latent_cache(jax.random.fold_in(splits[21], 71), 0)
    rotary_cache = normal_values(splits[6], (SEQS, CACHE, ROPE), 1.0, 6.0, ((0, 32),))
    lengths = draw_lengths(jax.random.fold_in(splits[21], 71), 0)
    value_up = normal_values(splits[8], (KL, H, V), (KL // 16) ** -0.5, 1.0)
    out_proj = normal_values(splits[9], (H * V, D), (H * V // 4) ** -0.5, 0.5)
    attn_gain = jnp.clip(1.0 + 0.18 * jax.random.normal(splits[10], (D,), jnp.float32), 0.099609375, 1.8984375).astype(jnp.bfloat16)
    mix_gate = normal_values(splits[11], (D,), D ** -0.5, 0.125)
    dense_w_gate = normal_values(splits[12], (D, FD), D ** -0.5, 0.125, ((1, 16),))
    dense_w_up = normal_values(splits[13], (D, FD), D ** -0.5, 0.125, ((1, 16),))
    dense_w_down = normal_values(splits[14], (FD, D), (FD // 16) ** -0.5, 0.5, ((0, 16),))
    expert_ids_keys = jax.random.split(jax.random.fold_in(splits[15], 1), SEQS // TOK_GROUP)
    expert_ids_turns = jax.random.permutation(jax.random.fold_in(splits[15], 3), SEQS // TOK_GROUP)
    expert_ids = jax.vmap(lambda own, number: routed_block(jax.random.fold_in(splits[15], 2), own, number, TOK_GROUP, EXPERTS, TOPK, CAP, 2))(expert_ids_keys, expert_ids_turns).reshape((SEQS, TOPK))
    expert_scores = jnp.clip(jnp.exp(math.log(5.0) - 3.912023 * jax.random.uniform(splits[16], (SEQS, TOPK), jnp.float32) ** steps_of(splits[16], (SEQS, TOPK), ((0, 32),), -0.2, 0.2)), 0.1, 5.0)
    expert_gate = normal_values(splits[17], (EXPERTS, D, FE), D ** -0.5, 0.125, ((0, 16), (2, 2)))
    expert_up = normal_values(splits[18], (EXPERTS, D, FE), D ** -0.5, 0.125, ((0, 16), (2, 2)))
    expert_down = normal_values(splits[19], (EXPERTS, FE, D), (FE // 16) ** -0.5, 1.0, ((0, 16), (1, 2)))
    out_gain = jnp.clip(1.0 + 0.18 * jax.random.normal(splits[20], (D,), jnp.float32), 0.099609375, 1.8984375).astype(jnp.bfloat16)
    return dict(residual=residual, query_latent=query_latent, query_rotary=query_rotary, latent_new=latent_new, rotary_new=rotary_new, latent_cache=latent_cache, rotary_cache=rotary_cache, lengths=lengths, value_up=value_up, out_proj=out_proj, attn_gain=attn_gain, mix_gate=mix_gate, dense_w_gate=dense_w_gate, dense_w_up=dense_w_up, dense_w_down=dense_w_down, expert_ids=expert_ids, expert_scores=expert_scores, expert_gate=expert_gate, expert_up=expert_up, expert_down=expert_down, out_gain=out_gain)


ALPHA = 8.0 ** 0.25
EPS = 1e-06
ROPE_BASE = 10000.0

def rotate(vector, position):
    half_dim = vector.shape[-1] // 2
    inv_freq = ROPE_BASE ** (-jnp.arange(half_dim, dtype=jnp.float32) / half_dim)
    angles = position.astype(jnp.float32)[..., None] * inv_freq
    cosine = jnp.cos(angles)
    sine_part = jnp.sin(angles)
    lower_half = vector[..., :half_dim]
    upper_half = vector[..., half_dim:]
    return jnp.concatenate([lower_half * cosine - upper_half * sine_part, upper_half * cosine + lower_half * sine_part], axis=-1)

def normalize(values, gain):
    center = lax.optimization_barrier(jnp.mean(values, -1, keepdims=True))
    spread = lax.optimization_barrier(jnp.mean(jnp.square(values - center), -1, keepdims=True))
    return (values - center) * lax.rsqrt(spread + EPS) * gain.astype(jnp.float32)

def attend(block):
    query_latent, query_rotary, latent_new, rotary_new, latent_cache, rotary_cache, lengths = block
    score_scale = (NOPE + ROPE) ** (-0.5)
    query_turned = rotate(query_rotary.astype(jnp.float32), lengths[:, None]).astype(jnp.bfloat16)
    key_turned = rotate(rotary_new.astype(jnp.float32), lengths).astype(jnp.bfloat16)
    query_wide = query_latent.astype(jnp.float32)
    turned_wide = query_turned.astype(jnp.float32)
    cache_wide = latent_cache.astype(jnp.float32)
    new_wide = latent_new.astype(jnp.float32)
    scores = (jnp.einsum('bhr,btr->bht', query_wide, cache_wide) + jnp.einsum('bhe,bte->bht', turned_wide, rotary_cache.astype(jnp.float32))) * score_scale
    own_score = (jnp.einsum('bhr,br->bh', query_wide, new_wide) + jnp.einsum('bhe,be->bh', turned_wide, key_turned.astype(jnp.float32))) * score_scale
    live = jnp.arange(CACHE, dtype=jnp.int32)[None, :] < lengths[:, None]
    scores = jnp.where(live[:, None, :], scores, -jnp.inf)
    top_score = jnp.maximum(lax.optimization_barrier(jnp.max(scores, -1)), own_score)
    cache_probs = jnp.exp(scores - top_score[..., None])
    own_prob = jnp.exp(own_score - top_score)
    prob_total = lax.optimization_barrier(jnp.sum(cache_probs, -1)) + own_prob
    cache_weights = (cache_probs / prob_total[..., None]).astype(jnp.bfloat16)
    own_weight = (own_prob / prob_total).astype(jnp.bfloat16)
    latent_out = jnp.einsum('bht,btr->bhr', cache_weights.astype(jnp.float32), cache_wide) + own_weight.astype(jnp.float32)[..., None] * new_wide[:, None, :]
    return latent_out.astype(jnp.bfloat16)

def expert_block(block):
    token_rows, gate_weight, up_weight, down_weight = block
    flat_rows = token_rows.reshape(-1, D)
    half_width = FE // N_TP
    summed = jnp.zeros(flat_rows.shape, jnp.float32)
    for part_index in range(N_TP):
        lower = part_index * half_width
        upper = lower + half_width
        gate_pre = jnp.dot(flat_rows, gate_weight[:, lower:upper], preferred_element_type=jnp.float32)
        up_pre = jnp.dot(flat_rows, up_weight[:, lower:upper], preferred_element_type=jnp.float32)
        hidden_part = (jax.nn.silu(gate_pre) * up_pre).astype(jnp.bfloat16)
        part_out = jnp.dot(hidden_part, down_weight[lower:upper], preferred_element_type=jnp.float32).astype(jnp.bfloat16)
        summed = summed + part_out.astype(jnp.float32)
    return summed.astype(jnp.bfloat16).reshape(token_rows.shape)

def reference(residual, query_latent, query_rotary, latent_new, rotary_new, latent_cache, rotary_cache, lengths, value_up, out_proj, attn_gain, mix_gate, dense_w_gate, dense_w_up, dense_w_down, expert_ids, expert_scores, expert_gate, expert_up, expert_down, out_gain):
    block_count = SEQS // SEQ_DEV

    def split_blocks(array):
        return array.reshape((block_count, SEQ_DEV) + array.shape[1:])
    latent_out = lax.map(attend, (split_blocks(query_latent), split_blocks(query_rotary), split_blocks(latent_new), split_blocks(rotary_new), split_blocks(latent_cache), split_blocks(rotary_cache), split_blocks(lengths)))
    latent_out = latent_out.reshape(SEQS, H, KL)
    heads_out = jnp.einsum('bhr,rhv->bhv', latent_out.astype(jnp.float32), value_up.astype(jnp.float32))
    heads_out = heads_out.astype(jnp.bfloat16).reshape(SEQS, H * V)
    attn = jnp.dot(heads_out, out_proj, preferred_element_type=jnp.float32).astype(jnp.bfloat16)
    mixed = normalize(ALPHA * residual.astype(jnp.float32) + attn.astype(jnp.float32), attn_gain).astype(jnp.bfloat16)
    mix = jax.nn.sigmoid(jnp.dot(mixed, mix_gate, preferred_element_type=jnp.float32))
    gate_pre = jnp.dot(mixed, dense_w_gate, preferred_element_type=jnp.float32)
    up_pre = jnp.dot(mixed, dense_w_up, preferred_element_type=jnp.float32)
    hidden = (jax.nn.silu(gate_pre) * up_pre).astype(jnp.bfloat16)
    dense_out = jnp.dot(hidden, dense_w_down, preferred_element_type=jnp.float32).astype(jnp.bfloat16)
    group_count = SEQS // TOK_GROUP
    route_ids = expert_ids.reshape(group_count, TOK_GROUP * TOPK)
    onehot = (route_ids[..., None] == jnp.arange(EXPERTS, dtype=jnp.int32)).astype(jnp.int32)
    slot_index = lax.optimization_barrier(jnp.sum((jnp.cumsum(onehot, 1) - 1) * onehot, -1)).astype(jnp.int32)
    group_index = jnp.broadcast_to(jnp.arange(group_count, dtype=jnp.int32)[:, None], route_ids.shape)
    token_rows = jnp.repeat(mixed.reshape(group_count, TOK_GROUP, D), TOPK, axis=1)
    buffer = jnp.zeros((EXPERTS, group_count, CAP, D), jnp.bfloat16).at[route_ids, group_index, slot_index].set(token_rows)
    expert_out = lax.map(expert_block, (buffer, expert_gate, expert_up, expert_down))
    picked = expert_out[route_ids, group_index, slot_index].reshape(SEQS, TOPK, D)
    share = expert_scores / lax.optimization_barrier(jnp.sum(expert_scores, 1, keepdims=True))
    routed = lax.optimization_barrier(jnp.sum(picked.astype(jnp.float32) * share[:, :, None], 1))
    summed_total = ALPHA * mixed.astype(jnp.float32) + routed + mix[:, None] * dense_out.astype(jnp.float32)
    return normalize(summed_total, out_gain).astype(jnp.bfloat16)
```

```python
import jax
import jax.numpy as jnp
from jax import lax
from jax.sharding import PartitionSpec as P

NOPE = 64
LANES = 128


ALPHA = 8.0**0.25
EPS = 1e-06
ROPE_BASE = 10000.0


def rotate(vector, position):
    half_dim = vector.shape[-1] // 2
    inv_freq = ROPE_BASE ** (-jnp.arange(half_dim, dtype=jnp.float32) / half_dim)
    angles = position.astype(jnp.float32)[..., None] * inv_freq
    cosine = jnp.cos(angles)
    sine_part = jnp.sin(angles)
    lower_half = vector[..., :half_dim]
    upper_half = vector[..., half_dim:]
    return jnp.concatenate(
        [
            lower_half * cosine - upper_half * sine_part,
            upper_half * cosine + lower_half * sine_part,
        ],
        axis=-1,
    )


def normalize(values, gain):
    center = jnp.mean(values, -1, keepdims=True)
    spread = jnp.mean(jnp.square(values - center), -1, keepdims=True)
    return (values - center) * lax.rsqrt(spread + EPS) * gain.astype(jnp.float32)


def gated(rows, gate_weight, up_weight, down_weight):
    gate_pre = jnp.dot(rows, gate_weight, preferred_element_type=jnp.float32)
    up_pre = jnp.dot(rows, up_weight, preferred_element_type=jnp.float32)
    hidden = (jax.nn.silu(gate_pre) * up_pre).astype(jnp.bfloat16)
    return jnp.dot(hidden, down_weight, preferred_element_type=jnp.float32)


def on_device(
    residual,
    query_latent,
    query_rotary,
    latent_new,
    rotary_new,
    latent_cache,
    rotary_cache,
    lengths,
    value_up,
    out_proj,
    attn_gain,
    mix_gate,
    dense_w_gate,
    dense_w_up,
    dense_w_down,
    expert_ids,
    expert_scores,
    expert_gate,
    expert_up,
    expert_down,
    out_gain,
):
    seq_count, model_width = residual.shape
    cache_len = latent_cache.shape[1]
    tp_count = lax.axis_size("tp")
    swap = [(i, (i + 1) % tp_count) for i in range(tp_count)]
    other_gate = lax.ppermute(expert_gate, "tp", swap)
    other_up = lax.ppermute(expert_up, "tp", swap)
    other_down = lax.ppermute(expert_down, "tp", swap)
    score_scale = (NOPE + query_rotary.shape[-1]) ** (-0.5)
    query_turned = rotate(query_rotary.astype(jnp.float32), lengths[:, None]).astype(jnp.bfloat16)
    key_turned = rotate(rotary_new.astype(jnp.float32), lengths).astype(jnp.bfloat16)
    scores = (
        jnp.einsum("bhr,btr->bht", query_latent, latent_cache, preferred_element_type=jnp.float32)
        + jnp.einsum("bhe,bte->bht", query_turned, rotary_cache, preferred_element_type=jnp.float32)
    ) * score_scale
    own_score = (
        jnp.einsum("bhr,br->bh", query_latent, latent_new, preferred_element_type=jnp.float32)
        + jnp.einsum("bhe,be->bh", query_turned, key_turned, preferred_element_type=jnp.float32)
    ) * score_scale
    live = jnp.arange(cache_len)[None, :] < lengths[:, None]
    scores = jnp.where(live[:, None, :], scores, -jnp.inf)
    top_score = jnp.maximum(jnp.max(scores, -1), own_score)
    cache_probs = jnp.exp(scores - top_score[..., None])
    own_prob = jnp.exp(own_score - top_score)
    prob_total = jnp.sum(cache_probs, -1) + own_prob
    cache_weights = (cache_probs / prob_total[..., None]).astype(jnp.bfloat16)
    own_weight = (own_prob / prob_total).astype(jnp.bfloat16)
    latent_out = (
        jnp.einsum("bht,btr->bhr", cache_weights, latent_cache, preferred_element_type=jnp.float32)
        + own_weight.astype(jnp.float32)[..., None] * latent_new.astype(jnp.float32)[:, None, :]
    ).astype(jnp.bfloat16)
    heads_out = jnp.einsum("bhr,rhv->bhv", latent_out, value_up, preferred_element_type=jnp.float32)
    heads_out = heads_out.astype(jnp.bfloat16).reshape(seq_count, -1)
    attn = jnp.dot(heads_out, out_proj, preferred_element_type=jnp.float32).astype(jnp.bfloat16)
    mixed = normalize(
        ALPHA * residual.astype(jnp.float32) + attn.astype(jnp.float32), attn_gain
    ).astype(jnp.bfloat16)
    ep_count = lax.axis_size("ep")
    route_share = expert_scores / jnp.sum(expert_scores, 1, keepdims=True)
    chosen = expert_ids[None] == jnp.arange(ep_count, dtype=jnp.int32)[:, None, None]
    weight_of = jnp.sum(jnp.where(chosen, route_share[None], 0.0), -1)
    coarse = lax.reduce_precision(weight_of, 8, 7)
    lane = lax.broadcasted_iota(jnp.int32, (ep_count, seq_count, LANES), 2)
    tail = jnp.where(
        lane == 0, coarse[..., None], jnp.where(lane == 1, (weight_of - coarse)[..., None], 0.0)
    ).astype(jnp.bfloat16)
    outgoing = jnp.concatenate(
        [jnp.broadcast_to(mixed[None], (ep_count, seq_count, model_width)), tail], -1
    )
    arrived = lax.all_to_all(outgoing, "ep", split_axis=0, concat_axis=0, tiled=True)
    arrived = arrived.reshape(ep_count * seq_count, model_width + LANES)
    rows = arrived[:, :model_width]
    weight = jnp.sum(arrived[:, model_width:].astype(jnp.float32), -1, keepdims=True)
    partial_value = gated(rows, expert_gate[0], expert_up[0], expert_down[0]) + gated(
        rows, other_gate[0], other_up[0], other_down[0]
    )
    mix = jax.nn.sigmoid(jnp.dot(rows, mix_gate, preferred_element_type=jnp.float32))
    dense_part = gated(rows, dense_w_gate, dense_w_up, dense_w_down)
    combined = (weight * partial_value + mix[:, None] * dense_part).astype(jnp.bfloat16)
    returned = lax.all_to_all(
        combined.reshape(ep_count, seq_count, model_width),
        "ep",
        split_axis=0,
        concat_axis=0,
        tiled=True,
    )
    summed_total = ALPHA * mixed.astype(jnp.float32) + jnp.sum(returned.astype(jnp.float32), 0)
    return normalize(summed_total, out_gain).astype(jnp.bfloat16)


def solution(mesh):
    return jax.shard_map(
        on_device,
        mesh=mesh,
        in_specs=(
            P(("ep", "tp"), None),
            P(("ep", "tp"), None, None),
            P(("ep", "tp"), None, None),
            P(("ep", "tp"), None),
            P(("ep", "tp"), None),
            P(("ep", "tp"), None, None),
            P(("ep", "tp"), None, None),
            P(("ep", "tp")),
            P(),
            P(),
            P(),
            P(),
            P(None, "ep"),
            P(None, "ep"),
            P("ep", None),
            P(("ep", "tp"), None),
            P(("ep", "tp"), None),
            P("ep", None, "tp"),
            P("ep", None, "tp"),
            P("ep", "tp", None),
            P(),
        ),
        out_specs=P(("ep", "tp"), None),
        check_vma=False,
    )
```

```python
import jax
import jax.numpy as jnp
from jax import lax
from jax.experimental import pallas as pl
from jax.experimental.pallas import tpu as pltpu
from jax.sharding import PartitionSpec as P

NOPE = 64
LANES = 128


ALPHA = 8.0**0.25
EPS = 1e-06
ROPE_BASE = 10000.0


def rotate(vector, position):
    half_dim = vector.shape[-1] // 2
    inv_freq = ROPE_BASE ** (-jnp.arange(half_dim, dtype=jnp.float32) / half_dim)
    angles = position.astype(jnp.float32)[..., None] * inv_freq
    cosine = jnp.cos(angles)
    sine_part = jnp.sin(angles)
    lower_half = vector[..., :half_dim]
    upper_half = vector[..., half_dim:]
    return jnp.concatenate(
        [
            lower_half * cosine - upper_half * sine_part,
            upper_half * cosine + lower_half * sine_part,
        ],
        axis=-1,
    )


def normalize(values, gain):
    center = jnp.mean(values, -1, keepdims=True)
    spread = jnp.mean(jnp.square(values - center), -1, keepdims=True)
    return (values - center) * lax.rsqrt(spread + EPS) * gain.astype(jnp.float32)


def branch_kernel(arrived, mix_gate, *refs):
    weights, out, held, total, sems = refs[:9], refs[9], refs[10:19], refs[19], refs[20]
    row_count, model_width = out.shape
    copies = [
        pltpu.make_async_copy(weights[i], held[i], sems.at[i]) for i in range(len(weights))
    ]
    for copy in copies:
        copy.start()
    block = min(row_count, 128)

    def stage(number):
        for copy in copies[3 * number : 3 * number + 3]:
            copy.wait()
        gate_weight, up_weight, down_weight = held[3 * number : 3 * number + 3]

        def piece(index, carry):
            place = pl.ds(pl.multiple_of(index * block, block), block)
            rows = arrived[place, :model_width]
            gate_pre = jnp.dot(rows, gate_weight[...], preferred_element_type=jnp.float32)
            up_pre = jnp.dot(rows, up_weight[...], preferred_element_type=jnp.float32)
            hidden = (jax.nn.silu(gate_pre) * up_pre).astype(jnp.bfloat16)
            part = jnp.dot(hidden, down_weight[...], preferred_element_type=jnp.float32)
            if number == 0:
                pre = rows.astype(jnp.float32) * mix_gate[...].astype(jnp.float32)
                total[place, :] = part * jax.nn.sigmoid(jnp.sum(pre, -1, keepdims=True))
            else:
                tail = arrived[place, model_width:].astype(jnp.float32)
                value = total[place, :] + part * jnp.sum(tail, -1, keepdims=True)
                if number == 1:
                    total[place, :] = value
                else:
                    out[place, :] = value.astype(jnp.bfloat16)
            return carry

        if row_count == block:
            piece(0, 0)
        else:
            lax.fori_loop(0, row_count // block, piece, 0)

    for number in range(3):
        stage(number)


def branches(arrived, mix_gate, weights, model_width):
    row_count = arrived.shape[0]
    return pl.pallas_call(
        branch_kernel,
        out_shape=jax.ShapeDtypeStruct((row_count, model_width), jnp.bfloat16),
        in_specs=[pl.BlockSpec(memory_space=pltpu.VMEM)] * 2
        + [pl.BlockSpec(memory_space=pl.ANY)] * len(weights),
        out_specs=pl.BlockSpec(memory_space=pltpu.VMEM),
        scratch_shapes=[pltpu.VMEM(weight.shape, weight.dtype) for weight in weights]
        + [
            pltpu.VMEM((row_count, model_width), jnp.float32),
            pltpu.SemaphoreType.DMA((len(weights),)),
        ],
        compiler_params=pltpu.CompilerParams(vmem_limit_bytes=56 << 20),
    )(arrived, mix_gate, *weights)


def on_device(
    residual,
    query_latent,
    query_rotary,
    latent_new,
    rotary_new,
    latent_cache,
    rotary_cache,
    lengths,
    value_up,
    out_proj,
    attn_gain,
    mix_gate,
    dense_w_gate,
    dense_w_up,
    dense_w_down,
    expert_ids,
    expert_scores,
    expert_gate,
    expert_up,
    expert_down,
    out_gain,
):
    seq_count, model_width = residual.shape
    cache_len = latent_cache.shape[1]
    tp_count = lax.axis_size("tp")
    swap = [(i, (i + 1) % tp_count) for i in range(tp_count)]
    other_gate = lax.ppermute(expert_gate, "tp", swap)
    other_up = lax.ppermute(expert_up, "tp", swap)
    other_down = lax.ppermute(expert_down, "tp", swap)
    score_scale = (NOPE + query_rotary.shape[-1]) ** (-0.5)
    query_turned = rotate(query_rotary.astype(jnp.float32), lengths[:, None]).astype(jnp.bfloat16)
    key_turned = rotate(rotary_new.astype(jnp.float32), lengths).astype(jnp.bfloat16)
    scores = (
        jnp.einsum("bhr,btr->bht", query_latent, latent_cache, preferred_element_type=jnp.float32)
        + jnp.einsum("bhe,bte->bht", query_turned, rotary_cache, preferred_element_type=jnp.float32)
    ) * score_scale
    own_score = (
        jnp.einsum("bhr,br->bh", query_latent, latent_new, preferred_element_type=jnp.float32)
        + jnp.einsum("bhe,be->bh", query_turned, key_turned, preferred_element_type=jnp.float32)
    ) * score_scale
    live = jnp.arange(cache_len)[None, :] < lengths[:, None]
    scores = jnp.where(live[:, None, :], scores, -jnp.inf)
    top_score = jnp.maximum(jnp.max(scores, -1), own_score)
    cache_probs = jnp.exp(scores - top_score[..., None])
    own_prob = jnp.exp(own_score - top_score)
    prob_total = jnp.sum(cache_probs, -1) + own_prob
    cache_weights = (cache_probs / prob_total[..., None]).astype(jnp.bfloat16)
    own_weight = (own_prob / prob_total).astype(jnp.bfloat16)
    latent_out = (
        jnp.einsum("bht,btr->bhr", cache_weights, latent_cache, preferred_element_type=jnp.float32)
        + own_weight.astype(jnp.float32)[..., None] * latent_new.astype(jnp.float32)[:, None, :]
    ).astype(jnp.bfloat16)
    heads_out = jnp.einsum("bhr,rhv->bhv", latent_out, value_up, preferred_element_type=jnp.float32)
    heads_out = heads_out.astype(jnp.bfloat16).reshape(seq_count, -1)
    attn = jnp.dot(heads_out, out_proj, preferred_element_type=jnp.float32).astype(jnp.bfloat16)
    mixed = normalize(
        ALPHA * residual.astype(jnp.float32) + attn.astype(jnp.float32), attn_gain
    ).astype(jnp.bfloat16)
    ep_count = lax.axis_size("ep")
    route_share = expert_scores / jnp.sum(expert_scores, 1, keepdims=True)
    chosen = expert_ids[None] == jnp.arange(ep_count, dtype=jnp.int32)[:, None, None]
    weight_of = jnp.sum(jnp.where(chosen, route_share[None], 0.0), -1)
    coarse = lax.reduce_precision(weight_of, 8, 7)
    lane = lax.broadcasted_iota(jnp.int32, (ep_count, seq_count, LANES), 2)
    tail = jnp.where(
        lane == 0, coarse[..., None], jnp.where(lane == 1, (weight_of - coarse)[..., None], 0.0)
    ).astype(jnp.bfloat16)
    outgoing = jnp.concatenate(
        [jnp.broadcast_to(mixed[None], (ep_count, seq_count, model_width)), tail], -1
    )
    arrived = lax.all_to_all(outgoing, "ep", split_axis=0, concat_axis=0, tiled=True)
    arrived = arrived.reshape(ep_count * seq_count, model_width + LANES)
    combined = branches(
        arrived,
        mix_gate[None],
        (
            dense_w_gate,
            dense_w_up,
            dense_w_down,
            expert_gate[0],
            expert_up[0],
            expert_down[0],
            other_gate[0],
            other_up[0],
            other_down[0],
        ),
        model_width,
    )
    returned = lax.all_to_all(
        combined.reshape(ep_count, seq_count, model_width),
        "ep",
        split_axis=0,
        concat_axis=0,
        tiled=True,
    )
    summed_total = ALPHA * mixed.astype(jnp.float32) + jnp.sum(returned.astype(jnp.float32), 0)
    return normalize(summed_total, out_gain).astype(jnp.bfloat16)


def solution(mesh):
    return jax.shard_map(
        on_device,
        mesh=mesh,
        in_specs=(
            P(("ep", "tp"), None),
            P(("ep", "tp"), None, None),
            P(("ep", "tp"), None, None),
            P(("ep", "tp"), None),
            P(("ep", "tp"), None),
            P(("ep", "tp"), None, None),
            P(("ep", "tp"), None, None),
            P(("ep", "tp")),
            P(),
            P(),
            P(),
            P(),
            P(None, "ep"),
            P(None, "ep"),
            P("ep", None),
            P(("ep", "tp"), None),
            P(("ep", "tp"), None),
            P("ep", None, "tp"),
            P("ep", None, "tp"),
            P("ep", "tp", None),
            P(),
        ),
        out_specs=P(("ep", "tp"), None),
        check_vma=False,
    )
```
